32 devices in a mesh: dp: 4 (over y, x), kv: 4 (over z), tp: 2 (over core).
Axes of the slice: x: 2, y: 2, z: 4, core: 2. Of those that a mesh axis runs over, the one named last changes fastest.
Arguments:
- tokens: bfloat16 [32, 4096], P('dp', ('kv', 'tp')), may hold values from -6 to 6
- w_query: bfloat16 [4096, 2, 1024], P(None, 'tp', 'kv'), may hold values from -0.09375 to 0.09375
- w_forget: bfloat16 [4096, 2, 1024], P(None, 'tp', 'kv'), may hold values from -0.09375 to 0.09375
- w_input: bfloat16 [4096, 2, 1024], P(None, 'tp', 'kv'), may hold values from -0.09375 to 0.09375
- w_output_gate: bfloat16 [4096, 2, 1024], P(None, 'tp', 'kv'), may hold values from -0.09375 to 0.09375
- gate_floor: float32 [2048], P('tp'), may hold values from 0 to 0.9
- head_gain: float32 [128], replicated, may hold values from 0.1 to 1.9
- w_out: bfloat16 [2048, 4096], P(None, ('kv', 'tp')), may hold values from -0.125 to 0.125
- mix_gain: float32 [4096], replicated, may hold values from 0.1 to 1.9
- ffn_gain: float32 [4096], replicated, may hold values from 0.1 to 1.9
- w_up: bfloat16 [4096, 16384], P(None, ('kv', 'tp')), may hold values from -0.09375 to 0.09375
- w_down: bfloat16 [16384, 4096], P(('kv', 'tp')), may hold values from -0.0625 to 0.0625
- state: float32 [32, 16, 128, 128], P(('dp', 'kv'), 'tp'), may hold values from -6 to 6
Outputs:
- mixed: bfloat16 [32, 4096], P('dp', ('kv', 'tp'))
- new_state: float32 [32, 16, 128, 128], P(('dp', 'kv'), 'tp')
The draws below stay inside these ranges and needn't reach their ends.
All inputs are finite; a program needn't handle non-finite values.
Results may differ from the reference program's by a relative error of at most 0.014.
Values may be sent and summed in bfloat16 or wider, within the bound.
A program may use at most 128 MiB of HBM per device.

```python
import jax
import jax.numpy as jnp
from jax import lax

D = 4096
HEADS = 16
HEAD = 128
FF = 16384
D_HG = 2048
BATCH = 32
N_TP = 2


def spiked(entries, stream_key, source, target, parts, factor):
    def block_of(position):
        return (jnp.arange(entries.shape[position]) // (entries.shape[position] // parts)).reshape((-1,) + (1,) * (entries.ndim - 1 - position))

    first = jax.random.permutation(stream_key, parts)[block_of(target)]
    second = (block_of(target) + parts // 2) % parts
    return jnp.where((block_of(source) == first) | (block_of(source) == second), factor * entries, entries)


def shard_levels(stream_key, shape, split, smallest, largest):
    def one(position, shards_of):
        heights = jax.random.uniform(jax.random.fold_in(jax.random.fold_in(stream_key, 6), position), (shards_of,), jnp.float32, smallest / len(split), largest / len(split))
        return jnp.repeat(jnp.exp(heights), shape[position] // shards_of).reshape((-1,) + (1,) * (len(shape) - position - 1))

    level = one(*split[0])
    for cut in split[1:]:
        level = level * one(*cut)
    return level


def gaussian(key, shape, scale, reach, cuts=(), held_as=jnp.bfloat16):
    drawn = scale * jax.random.normal(key, shape, jnp.float32)
    if cuts:
        drawn = drawn * shard_levels(key, shape, cuts, -0.22, 0.18)
    return jnp.clip(drawn, -reach, reach).astype(held_as)


def heavy_noise(rng, dims, deviation, limit, cuts, heavy, kind=jnp.bfloat16):
    result = deviation * jax.random.normal(rng, dims, jnp.float32)
    if cuts:
        result = result * shard_levels(rng, dims, cuts, -0.22, 0.18)
    return jnp.clip(spiked(result, jax.random.fold_in(rng, 3), *heavy), -limit, limit).astype(kind)


def setup_inputs(seed: int = 0) -> dict:
    key_of = jax.random.split(jax.random.key(seed), 14)
    return {
        "tokens": gaussian(key_of[0], (BATCH, D), 1.0, 6.0, ((0, 4), (1, 8))),
        "w_query": gaussian(key_of[1], (D, N_TP, D_HG // N_TP), D ** -0.5, 0.09375, ((1, 2), (2, 4))),
        "w_forget": gaussian(key_of[2], (D, N_TP, D_HG // N_TP), D ** -0.5, 0.09375, ((1, 2), (2, 4))),
        "w_input": gaussian(key_of[3], (D, N_TP, D_HG // N_TP), D ** -0.5, 0.09375, ((1, 2), (2, 4))),
        "w_output_gate": gaussian(key_of[4], (D, N_TP, D_HG // N_TP), D ** -0.5, 0.09375, ((1, 2), (2, 4))),
        "gate_floor": jnp.clip(0.9 * jax.random.uniform(key_of[5], (D_HG,), jnp.float32) ** shard_levels(key_of[5], (D_HG,), ((0, 2),), -0.2, 0.2), 0.0, 0.9),
        "head_gain": jnp.clip(1.0 + 0.18 * jax.random.normal(key_of[6], (HEAD,), jnp.float32), 0.1, 1.9),
        "w_out": gaussian(key_of[7], (D_HG, D), D_HG ** -0.5, 0.125, ((1, 8),)),
        "mix_gain": jnp.clip(1.0 + 0.18 * jax.random.normal(key_of[8], (D,), jnp.float32), 0.1, 1.9),
        "ffn_gain": jnp.clip(1.0 + 0.18 * jax.random.normal(key_of[9], (D,), jnp.float32), 0.1, 1.9),
        "w_up": gaussian(key_of[10], (D, FF), D ** -0.5, 0.09375, ((1, 8),)),
        "w_down": heavy_noise(key_of[11], (FF, D), FF ** -0.5, 0.0625, ((0, 8),), (0, 1, 8, 2.0)),
        "state": gaussian(key_of[12], (BATCH, HEADS, HEAD, HEAD), 1.0, 6.0, ((0, 16), (1, 2)), jnp.float32),
    }


EPSILON = 1e-06

def rms_scale(values, gain):
    return values * lax.rsqrt(lax.optimization_barrier(jnp.mean(values * values, axis=-1, keepdims=True)) + EPSILON) * gain

def reference(tokens, w_query, w_forget, w_input, w_output_gate, gate_floor, head_gain, w_out, mix_gain, ffn_gain, w_up, w_down, state):
    tokens_f = tokens.astype(jnp.float32)
    normed = rms_scale(tokens_f, mix_gain).astype(jnp.bfloat16)

    def project(weight):
        return jnp.dot(normed, weight.reshape(D, D_HG), preferred_element_type=jnp.float32).astype(jnp.bfloat16)
    batch_rows = tokens.shape[0]
    query_raw = project(w_query).astype(jnp.float32).reshape(batch_rows, HEADS, HEAD)
    forget_raw = project(w_forget).astype(jnp.float32).reshape(batch_rows, HEADS, HEAD)
    input_vec = project(w_input).astype(jnp.float32).reshape(batch_rows, HEADS, HEAD)
    gate_raw = project(w_output_gate).astype(jnp.float32).reshape(batch_rows, HEADS, HEAD)
    query_vec = query_raw * HEAD ** (-0.5)
    floor_heads = gate_floor.reshape(HEADS, HEAD)
    forget_gate = floor_heads + (1.0 - floor_heads) * jax.nn.sigmoid(forget_raw)
    new_state = forget_gate[..., None] * state + (1.0 - forget_gate)[..., None] * input_vec[:, :, None, :]
    head_out = jnp.einsum('bhk,bhkv->bhv', query_vec, new_state, precision=lax.Precision.HIGHEST)
    branch = rms_scale(head_out, head_gain) * jax.nn.silu(gate_raw)
    branch = branch.reshape(batch_rows, D_HG).astype(jnp.bfloat16)
    residual_one = (tokens_f + jnp.dot(branch, w_out, preferred_element_type=jnp.float32)).astype(jnp.bfloat16)
    residual_f = residual_one.astype(jnp.float32)
    ffn_in = rms_scale(residual_f, ffn_gain).astype(jnp.bfloat16)
    upward = jnp.dot(ffn_in, w_up, preferred_element_type=jnp.float32)
    hidden = jnp.square(jax.nn.relu(upward)).astype(jnp.bfloat16)
    mixed = (residual_f + jnp.dot(hidden, w_down, preferred_element_type=jnp.float32)).astype(jnp.bfloat16)
    return (mixed, new_state)
```

```python
import functools

import jax
import jax.numpy as jnp
from jax import lax
from jax.experimental import pallas as pl
from jax.experimental.pallas import tpu as pltpu
from jax.sharding import PartitionSpec as P

EPSILON = 1e-06


def rms_scale(values, gain):
    return values * lax.rsqrt(jnp.mean(values * values, axis=-1, keepdims=True) + EPSILON) * gain


def per_device(
    tokens,
    w_query,
    w_forget,
    w_input,
    w_output_gate,
    gate_floor,
    head_gain,
    w_out,
    mix_gain,
    ffn_gain,
    w_up,
    w_down,
    state,
):
    group_kv = lax.axis_size("kv")
    group_tp = lax.axis_size("tp")
    tokens_f = tokens.astype(jnp.float32)
    full_rows = lax.all_gather(tokens, ("kv", "tp"), axis=1, tiled=True)
    normed = rms_scale(full_rows.astype(jnp.float32), mix_gain).astype(jnp.bfloat16)

    def project(weight):
        return jnp.dot(normed, weight[:, 0, :], preferred_element_type=jnp.float32).astype(
            jnp.bfloat16
        )

    query_raw, forget_raw, input_raw, gate_raw = (
        lax.all_to_all(project(w_query), "kv", split_axis=0, concat_axis=1, tiled=True),
        lax.all_to_all(project(w_forget), "kv", split_axis=0, concat_axis=1, tiled=True),
        lax.all_to_all(project(w_input), "kv", split_axis=0, concat_axis=1, tiled=True),
        lax.all_to_all(project(w_output_gate), "kv", split_axis=0, concat_axis=1, tiled=True),
    )
    seq_local = state.shape[0]
    heads_local = state.shape[1]
    head_size = state.shape[2]
    query_vec = query_raw.astype(jnp.float32).reshape(
        seq_local, heads_local, head_size
    ) * head_size ** (-0.5)
    floor_heads = gate_floor.reshape(heads_local, head_size)
    forget_gate = floor_heads + (1.0 - floor_heads) * jax.nn.sigmoid(
        forget_raw.astype(jnp.float32).reshape(seq_local, heads_local, head_size)
    )
    input_vec = input_raw.astype(jnp.float32).reshape(seq_local, heads_local, head_size)
    gate_vec = gate_raw.astype(jnp.float32).reshape(seq_local, heads_local, head_size)
    new_state = (
        forget_gate[..., None] * state + (1.0 - forget_gate)[..., None] * input_vec[:, :, None, :]
    )
    head_out = jnp.einsum("bhk,bhkv->bhv", query_vec, new_state, precision=lax.Precision.HIGHEST)
    branch = rms_scale(head_out, head_gain) * jax.nn.silu(gate_vec)
    branch = branch.reshape(seq_local, 1, heads_local * head_size).astype(jnp.bfloat16)
    gathered = lax.all_gather(branch, ("kv", "tp"), axis=1, tiled=True)
    gathered = gathered.reshape(seq_local, group_kv, group_tp, heads_local * head_size)
    gathered = jnp.transpose(gathered, (1, 0, 2, 3)).reshape(
        group_kv * seq_local, group_tp * heads_local * head_size
    )
    projected = jnp.dot(gathered, w_out, preferred_element_type=jnp.float32)
    residual_one = (tokens_f + projected).astype(jnp.bfloat16)
    whole_rows = lax.all_gather(residual_one, ("kv", "tp"), axis=1, tiled=True)
    ffn_in = rms_scale(whole_rows.astype(jnp.float32), ffn_gain).astype(jnp.bfloat16)
    upward = jnp.dot(ffn_in, w_up, preferred_element_type=jnp.float32)
    hidden = jnp.square(jax.nn.relu(upward)).astype(jnp.bfloat16)
    partial_terms = jnp.dot(hidden, w_down, preferred_element_type=jnp.float32)
    summed = lax.psum_scatter(partial_terms, ("kv", "tp"), scatter_dimension=1, tiled=True)
    results = (residual_one.astype(jnp.float32) + summed).astype(jnp.bfloat16)
    return (results, new_state)


MESH = pl.DeviceIdType.MESH
LANES = 128
VMEM_BUDGET = 60 * 1024 * 1024
PIECES = 4


def fused_kernel(
    n_kv,
    n_tp,
    tokens,
    w_query,
    w_forget,
    w_input,
    w_gate,
    gate_floor,
    head_gain,
    w_out,
    mix_gain,
    ffn_gain,
    w_up,
    w_down,
    state,
    mixed,
    new_state,
    rows_all,
    residual_all,
    projections,
    out_weight,
    up_weight,
    down_weight,
    state_buf,
    floor_buf,
    head_gain_buf,
    mix_gain_buf,
    ffn_gain_buf,
    normed,
    proj_send,
    proj_recv,
    vectors,
    head_buf,
    branch_send,
    branch_recv,
    branch_all,
    hidden,
    sum_send,
    sum_recv,
    mixed_buf,
    small_sem,
    proj_sem,
    out_sem,
    up_sem,
    down_sem,
    state_sem,
    result_sem,
    send_sem,
    recv_sem,
):
    group = n_kv * n_tp
    kv = lax.axis_index("kv")
    tp = lax.axis_index("tp")
    me = kv * n_tp + tp
    order = sorted(range(1, group), key=lambda r: -min(r, group - r))

    def peer(r):
        return lax.rem(me + r, group)

    def device_of(index):
        return {"kv": index // n_tp, "tp": lax.rem(index, n_tp)}

    rows, width = tokens.shape
    seqs, heads, size, _ = state.shape
    proj_cols = w_query.shape[1]
    heads_each = proj_cols // size
    model = group * width

    def load(source, target, sem):
        copy = pltpu.make_async_copy(source, target, sem)
        copy.start()
        return copy

    token_load = load(tokens, rows_all.at[me], small_sem.at[0])
    mix_load = load(mix_gain, mix_gain_buf, small_sem.at[1])
    proj_loads = [
        load(w, projections.at[i], proj_sem.at[i])
        for i, w in enumerate((w_query, w_forget, w_input, w_gate))
    ]
    floor_load = load(gate_floor, floor_buf, small_sem.at[2])
    gain_load = load(head_gain, head_gain_buf, small_sem.at[3])
    ffn_load = load(ffn_gain, ffn_gain_buf, small_sem.at[4])
    state_load = load(state, state_buf, state_sem.at[0])
    out_load = load(w_out, out_weight, out_sem.at[0])

    def pieces(source, target, sems):
        depth = source.shape[0] // PIECES
        return [
            load(
                source.at[pl.ds(i * depth, depth)],
                target.at[pl.ds(i * depth, depth)],
                sems.at[i],
            )
            for i in range(PIECES)
        ]

    up_loads = pieces(w_up, up_weight, up_sem)
    down_loads = pieces(w_down, down_weight, down_sem)

    barrier = pltpu.get_barrier_semaphore()
    for r in range(1, group):
        pl.semaphore_signal(
            barrier, inc=1, device_id=device_of(peer(r)), device_id_type=MESH
        )
    pl.semaphore_wait(barrier, group - 1)

    def send(phase, slot, source, target, device):
        copy = pltpu.make_async_remote_copy(
            src_ref=source,
            dst_ref=target,
            send_sem=send_sem.at[phase, slot],
            recv_sem=recv_sem.at[phase, slot],
            device_id=device,
            device_id_type=MESH,
        )
        copy.start()
        return copy

    def norm_rows(buffer, gain_ref):
        parts = [buffer[s].astype(jnp.float32) for s in range(group)]
        total = parts[0] * parts[0]
        for part in parts[1:]:
            total = total + part * part
        scale = lax.rsqrt(jnp.sum(total, axis=-1, keepdims=True) / model + EPSILON)
        for s in range(group):
            columns = slice(s * width, (s + 1) * width)
            normed[:, columns] = (parts[s] * scale * gain_ref[:, columns]).astype(
                jnp.bfloat16
            )

    token_load.wait()
    sends = [
        send(0, r, rows_all.at[me], rows_all.at[me], device_of(peer(r))) for r in order
    ]
    mix_load.wait()
    for copy in sends:
        copy.wait_recv()
    norm_rows(rows_all, mix_gain_buf)

    for i in range(4):
        proj_loads[i].wait()
        product = jnp.dot(
            normed[...], projections[i], preferred_element_type=jnp.float32
        )
        product = product.astype(jnp.bfloat16).astype(jnp.float32)
        for s in range(n_kv):
            for j in range(heads_each):
                proj_send[s, i, j] = product[
                    s * seqs : (s + 1) * seqs, j * size : (j + 1) * size
                ]
    exchange = []
    for r in sorted(range(1, n_kv), key=lambda r: -min(r, n_kv - r)):
        other = lax.rem(kv + r, n_kv)
        exchange.append(
            send(1, r, proj_send.at[other], proj_recv.at[kv], {"kv": other, "tp": tp})
        )
    own = pltpu.make_async_copy(proj_send.at[kv], proj_recv.at[kv], small_sem.at[5])
    own.start()
    floor_load.wait()
    gain_load.wait()
    state_load.wait()
    own.wait()
    for copy in exchange:
        copy.wait_recv()

    for i in range(4):
        for s in range(n_kv):
            for j in range(heads_each):
                piece = proj_recv[s, i, j]
                for b in range(seqs):
                    row = b * heads + s * heads_each + j
                    vectors[i, row : row + 1, :] = piece[b : b + 1, :]

    floor = jnp.concatenate([floor_buf[...]] * seqs, axis=0)
    forget = floor + (1.0 - floor) * jax.nn.sigmoid(vectors[1])
    forget_t = forget.T
    query_t = (vectors[0] * size ** (-0.5)).T
    for b in range(seqs):
        for h in range(heads):
            row = b * heads + h
            f = jnp.broadcast_to(forget_t[:, row : row + 1], (size, size))
            q = jnp.broadcast_to(query_t[:, row : row + 1], (size, size))
            value = vectors[2, row : row + 1, :]
            updated = f * state_buf[b, h] + (1.0 - f) * value
            state_buf[b, h] = updated
            head_buf[row : row + 1, :] = jnp.sum(q * updated, axis=0, keepdims=True)
    heads_out = head_buf[...]
    gate = vectors[3]
    branch = (
        heads_out
        * lax.rsqrt(jnp.mean(heads_out * heads_out, axis=-1, keepdims=True) + EPSILON)
        * head_gain_buf[...]
        * (gate * jax.nn.sigmoid(gate))
    )
    branch = branch.astype(jnp.bfloat16).astype(jnp.float32)
    for b in range(seqs):
        for h in range(heads):
            row = b * heads + h
            branch_send[b : b + 1, h * size : (h + 1) * size] = branch[row : row + 1, :]
    branch_copies = [
        send(2, r, branch_send, branch_recv.at[kv, tp], device_of(peer(r)))
        for r in order
    ]
    own_branch = pltpu.make_async_copy(
        branch_send, branch_recv.at[kv, tp], small_sem.at[6]
    )
    own_branch.start()
    state_store = load(state_buf, new_state, result_sem.at[0])
    out_load.wait()
    own_branch.wait()
    for copy in branch_copies:
        copy.wait_recv()
    for s in range(n_kv):
        for t in range(n_tp):
            branch_all[
                s * seqs : (s + 1) * seqs, t * heads * size : (t + 1) * heads * size
            ] = branch_recv[s, t]
    projected = jnp.dot(
        branch_all[...].astype(jnp.bfloat16),
        out_weight[...],
        preferred_element_type=jnp.float32,
    )
    residual_all[me] = (rows_all[me].astype(jnp.float32) + projected).astype(
        jnp.bfloat16
    )
    residual_copies = [
        send(3, r, residual_all.at[me], residual_all.at[me], device_of(peer(r)))
        for r in order
    ]
    ffn_load.wait()
    for copy in residual_copies:
        copy.wait_recv()
    norm_rows(residual_all, ffn_gain_buf)

    for copy in up_loads:
        copy.wait()
    hidden_cols = w_up.shape[1]
    step = min(512, hidden_cols)

    def up_step(j, carry):
        columns = pl.ds(pl.multiple_of(j * step, step), step)
        upward = jnp.dot(
            normed[...], up_weight[:, columns], preferred_element_type=jnp.float32
        )
        upward = jnp.maximum(upward, 0.0)
        hidden[:, columns] = (upward * upward).astype(jnp.bfloat16)
        return carry

    lax.fori_loop(0, hidden_cols // step, up_step, 0)

    for copy in down_loads:
        copy.wait()

    def down(index):
        columns = pl.ds(pl.multiple_of(index * width, width), width)
        return jnp.dot(
            hidden[...], down_weight[:, columns], preferred_element_type=jnp.float32
        )

    sum_copies = []
    for r in order:
        sum_send[r] = down(peer(r)).astype(jnp.bfloat16)
        sum_copies.append(
            send(4, r, sum_send.at[r], sum_recv.at[r], device_of(peer(r)))
        )
    total = down(me)
    for copy in sum_copies:
        copy.wait_recv()
    for r in range(1, group):
        total = total + sum_recv[r].astype(jnp.float32)
    mixed_buf[...] = (residual_all[me].astype(jnp.float32) + total).astype(jnp.bfloat16)
    mixed_store = load(mixed_buf, mixed, result_sem.at[1])
    for copy in sends + exchange + branch_copies + residual_copies + sum_copies:
        copy.wait_send()
    state_store.wait()
    mixed_store.wait()


def fused_scratch(n_kv, n_tp, tokens, w_query, w_out, w_up, w_down, state):
    group = n_kv * n_tp
    rows, width = tokens.shape
    seqs, heads, size, _ = state.shape
    heads_each = w_query.shape[2] // size
    bf16, f32 = jnp.bfloat16, jnp.float32
    return [
        pltpu.VMEM((group, rows, width), bf16),
        pltpu.VMEM((group, rows, width), bf16),
        pltpu.VMEM((4, w_query.shape[0], w_query.shape[2]), bf16),
        pltpu.VMEM(w_out.shape, bf16),
        pltpu.VMEM(w_up.shape, bf16),
        pltpu.VMEM(w_down.shape, bf16),
        pltpu.VMEM(state.shape, f32),
        pltpu.VMEM((heads, size), f32),
        pltpu.VMEM((1, size), f32),
        pltpu.VMEM((1, group * width), f32),
        pltpu.VMEM((1, group * width), f32),
        pltpu.VMEM((rows, group * width), bf16),
        pltpu.VMEM((n_kv, 4, heads_each, seqs, size), f32),
        pltpu.VMEM((n_kv, 4, heads_each, seqs, size), f32),
        pltpu.VMEM((4, seqs * heads, size), f32),
        pltpu.VMEM((seqs * heads, size), f32),
        pltpu.VMEM((seqs, heads * size), f32),
        pltpu.VMEM((n_kv, n_tp, seqs, heads * size), f32),
        pltpu.VMEM((rows, n_tp * heads * size), f32),
        pltpu.VMEM((rows, w_up.shape[1]), bf16),
        pltpu.VMEM((group, rows, width), bf16),
        pltpu.VMEM((group, rows, width), bf16),
        pltpu.VMEM((rows, width), bf16),
        pltpu.SemaphoreType.DMA((7,)),
        pltpu.SemaphoreType.DMA((4,)),
        pltpu.SemaphoreType.DMA((1,)),
        pltpu.SemaphoreType.DMA((PIECES,)),
        pltpu.SemaphoreType.DMA((PIECES,)),
        pltpu.SemaphoreType.DMA((1,)),
        pltpu.SemaphoreType.DMA((2,)),
        pltpu.SemaphoreType.DMA((5, group)),
        pltpu.SemaphoreType.DMA((5, group)),
    ]


def fused(
    tokens,
    w_query,
    w_forget,
    w_input,
    w_output_gate,
    gate_floor,
    head_gain,
    w_out,
    mix_gain,
    ffn_gain,
    w_up,
    w_down,
    state,
):
    n_kv = lax.axis_size("kv")
    n_tp = lax.axis_size("tp")
    anywhere = pl.BlockSpec(memory_space=pl.ANY)
    size = state.shape[2]
    return pl.pallas_call(
        functools.partial(fused_kernel, n_kv, n_tp),
        out_shape=(
            jax.ShapeDtypeStruct(tokens.shape, jnp.bfloat16),
            jax.ShapeDtypeStruct(state.shape, jnp.float32),
        ),
        in_specs=[anywhere] * 13,
        out_specs=(anywhere, anywhere),
        scratch_shapes=fused_scratch(
            n_kv, n_tp, tokens, w_query, w_out, w_up, w_down, state
        ),
        compiler_params=pltpu.CompilerParams(
            collective_id=0, has_side_effects=True, vmem_limit_bytes=VMEM_BUDGET
        ),
    )(
        tokens,
        w_query[:, 0, :],
        w_forget[:, 0, :],
        w_input[:, 0, :],
        w_output_gate[:, 0, :],
        gate_floor.reshape(state.shape[1], size),
        head_gain.reshape(1, size),
        w_out,
        mix_gain.reshape(1, -1),
        ffn_gain.reshape(1, -1),
        w_up,
        w_down,
        state,
    )


def dispatch(*operands):
    tokens, w_query, w_out, w_up, w_down, state = (
        operands[0],
        operands[1],
        operands[7],
        operands[10],
        operands[11],
        operands[12],
    )
    weights = 2 * (4 * w_query.size + w_out.size + w_up.size + w_down.size)
    held = weights + 4 * state.size + 64 * tokens.size * lax.axis_size("kv")
    size = state.shape[2]
    if (
        held <= VMEM_BUDGET
        and size == LANES
        and w_query.shape[2] % size == 0
        and tokens.shape[0] == lax.axis_size("kv") * state.shape[0]
        and tokens.shape[0] <= 64
    ):
        return fused(*operands)
    return per_device(*operands)


def solution(mesh):
    placed = (
        P("dp", ("kv", "tp")),
        P(None, "tp", "kv"),
        P(None, "tp", "kv"),
        P(None, "tp", "kv"),
        P(None, "tp", "kv"),
        P("tp"),
        P(),
        P(None, ("kv", "tp")),
        P(),
        P(),
        P(None, ("kv", "tp")),
        P(("kv", "tp"), None),
        P(("dp", "kv"), "tp", None, None),
    )
    return jax.shard_map(
        dispatch,
        mesh=mesh,
        in_specs=placed,
        out_specs=(P("dp", ("kv", "tp")), P(("dp", "kv"), "tp", None, None)),
        check_vma=False,
    )
```

```python
import functools

import jax
import jax.numpy as jnp
from jax import lax
from jax.experimental import pallas as pl
from jax.experimental.pallas import tpu as pltpu
from jax.sharding import PartitionSpec as P

EPSILON = 1e-06


def rms_scale(values, gain):
    return values * lax.rsqrt(jnp.mean(values * values, axis=-1, keepdims=True) + EPSILON) * gain


def per_device(
    tokens,
    w_query,
    w_forget,
    w_input,
    w_output_gate,
    gate_floor,
    head_gain,
    w_out,
    mix_gain,
    ffn_gain,
    w_up,
    w_down,
    state,
):
    group_kv = lax.axis_size("kv")
    group_tp = lax.axis_size("tp")
    tokens_f = tokens.astype(jnp.float32)
    full_rows = lax.all_gather(tokens, ("kv", "tp"), axis=1, tiled=True)
    normed = rms_scale(full_rows.astype(jnp.float32), mix_gain).astype(jnp.bfloat16)

    def project(weight):
        return jnp.dot(normed, weight[:, 0, :], preferred_element_type=jnp.float32).astype(
            jnp.bfloat16
        )

    query_raw, forget_raw, input_raw, gate_raw = (
        lax.all_to_all(project(w_query), "kv", split_axis=0, concat_axis=1, tiled=True),
        lax.all_to_all(project(w_forget), "kv", split_axis=0, concat_axis=1, tiled=True),
        lax.all_to_all(project(w_input), "kv", split_axis=0, concat_axis=1, tiled=True),
        lax.all_to_all(project(w_output_gate), "kv", split_axis=0, concat_axis=1, tiled=True),
    )
    seq_local = state.shape[0]
    heads_local = state.shape[1]
    head_size = state.shape[2]
    query_vec = query_raw.astype(jnp.float32).reshape(
        seq_local, heads_local, head_size
    ) * head_size ** (-0.5)
    floor_heads = gate_floor.reshape(heads_local, head_size)
    forget_gate = floor_heads + (1.0 - floor_heads) * jax.nn.sigmoid(
        forget_raw.astype(jnp.float32).reshape(seq_local, heads_local, head_size)
    )
    input_vec = input_raw.astype(jnp.float32).reshape(seq_local, heads_local, head_size)
    gate_vec = gate_raw.astype(jnp.float32).reshape(seq_local, heads_local, head_size)
    new_state = (
        forget_gate[..., None] * state + (1.0 - forget_gate)[..., None] * input_vec[:, :, None, :]
    )
    head_out = jnp.einsum("bhk,bhkv->bhv", query_vec, new_state, precision=lax.Precision.HIGHEST)
    branch = rms_scale(head_out, head_gain) * jax.nn.silu(gate_vec)
    branch = branch.reshape(seq_local, 1, heads_local * head_size).astype(jnp.bfloat16)
    gathered = lax.all_gather(branch, ("kv", "tp"), axis=1, tiled=True)
    gathered = gathered.reshape(seq_local, group_kv, group_tp, heads_local * head_size)
    gathered = jnp.transpose(gathered, (1, 0, 2, 3)).reshape(
        group_kv * seq_local, group_tp * heads_local * head_size
    )
    projected = jnp.dot(gathered, w_out, preferred_element_type=jnp.float32)
    residual_one = (tokens_f + projected).astype(jnp.bfloat16)
    whole_rows = lax.all_gather(residual_one, ("kv", "tp"), axis=1, tiled=True)
    ffn_in = rms_scale(whole_rows.astype(jnp.float32), ffn_gain).astype(jnp.bfloat16)
    upward = jnp.dot(ffn_in, w_up, preferred_element_type=jnp.float32)
    hidden = jnp.square(jax.nn.relu(upward)).astype(jnp.bfloat16)
    partial_terms = jnp.dot(hidden, w_down, preferred_element_type=jnp.float32)
    summed = lax.psum_scatter(partial_terms, ("kv", "tp"), scatter_dimension=1, tiled=True)
    results = (residual_one.astype(jnp.float32) + summed).astype(jnp.bfloat16)
    return (results, new_state)


MESH = pl.DeviceIdType.MESH
LANES = 128
VMEM_BUDGET = 60 * 1024 * 1024
PIECES = 4


def fused_kernel(
    n_kv,
    n_tp,
    tokens,
    w_query,
    w_forget,
    w_input,
    w_gate,
    gate_floor,
    head_gain,
    w_out,
    mix_gain,
    ffn_gain,
    w_up,
    w_down,
    state,
    mixed,
    new_state,
    rows_all,
    residual_all,
    projections,
    out_weight,
    up_weight,
    down_weight,
    state_buf,
    floor_buf,
    head_gain_buf,
    mix_gain_buf,
    ffn_gain_buf,
    proj_send,
    proj_recv,
    vectors,
    head_buf,
    branch_send,
    branch_recv,
    branch_all,
    hidden,
    sum_send,
    sum_recv,
    small_sem,
    proj_sem,
    out_sem,
    up_sem,
    down_sem,
    state_sem,
    send_sem,
    recv_sem,
):
    group = n_kv * n_tp
    kv = lax.axis_index("kv")
    tp = lax.axis_index("tp")
    me = kv * n_tp + tp
    order = sorted(range(1, group), key=lambda r: -min(r, group - r))

    def peer(r):
        return lax.rem(me + r, group)

    def device_of(index):
        return {"kv": index // n_tp, "tp": lax.rem(index, n_tp)}

    rows, width = tokens.shape
    seqs, heads, size, _ = state.shape
    proj_cols = w_query.shape[1]
    heads_each = proj_cols // size
    model = group * width

    def load(source, target, sem):
        copy = pltpu.make_async_copy(source, target, sem)
        copy.start()
        return copy

    token_load = load(tokens, rows_all.at[me], small_sem.at[0])
    mix_load = load(mix_gain, mix_gain_buf, small_sem.at[1])
    proj_loads = [
        load(w, projections.at[i], proj_sem.at[i])
        for i, w in enumerate((w_query, w_forget, w_input, w_gate))
    ]
    floor_load = load(gate_floor, floor_buf, small_sem.at[2])
    gain_load = load(head_gain, head_gain_buf, small_sem.at[3])
    ffn_load = load(ffn_gain, ffn_gain_buf, small_sem.at[4])
    state_load = load(state, state_buf, state_sem.at[0])
    out_load = load(w_out, out_weight, out_sem.at[0])

    def pieces(source, target, sems):
        depth = source.shape[0] // PIECES
        return [
            load(
                source.at[pl.ds(i * depth, depth)],
                target.at[pl.ds(i * depth, depth)],
                sems.at[i],
            )
            for i in range(PIECES)
        ]

    barrier = pltpu.get_barrier_semaphore()
    for r in range(1, group):
        pl.semaphore_signal(
            barrier, inc=1, device_id=device_of(peer(r)), device_id_type=MESH
        )
    pl.semaphore_wait(barrier, group - 1)

    def send(phase, slot, source, target, device):
        copy = pltpu.make_async_remote_copy(
            src_ref=source,
            dst_ref=target,
            send_sem=send_sem.at[phase, slot],
            recv_sem=recv_sem.at[phase, slot],
            device_id=device,
            device_id_type=MESH,
        )
        copy.start()
        return copy

    def gathered_dot(buffer, gain_ref, copies, weight_of):
        arrivals = [(me, None)] + [
            (lax.rem(me + group - r, group), copy)
            for r, copy in reversed(list(zip(order, copies)))
        ]
        sums = None
        squares = None
        for source, copy in arrivals:
            if copy is not None:
                copy.wait_recv()
            columns = pl.ds(pl.multiple_of(source * width, width), width)
            part = buffer[source].astype(jnp.float32)
            square = part * part
            squares = square if squares is None else squares + square
            scaled = (part * gain_ref[:, columns]).astype(jnp.bfloat16)
            terms = [
                jnp.dot(scaled, block, preferred_element_type=jnp.float32)
                for block in weight_of(columns)
            ]
            sums = terms if sums is None else [a + b for a, b in zip(sums, terms)]
        scale = lax.rsqrt(jnp.sum(squares, axis=-1, keepdims=True) / model + EPSILON)
        return [total * scale for total in sums]

    token_load.wait()
    sends = [
        send(0, r, rows_all.at[me], rows_all.at[me], device_of(peer(r))) for r in order
    ]
    mix_load.wait()
    for copy in proj_loads:
        copy.wait()
    up_loads = pieces(w_up, up_weight, up_sem)
    down_loads = pieces(w_down, down_weight, down_sem)
    products = gathered_dot(
        rows_all,
        mix_gain_buf,
        sends,
        lambda rows_at: [projections[i, rows_at, :] for i in range(4)],
    )
    for i, product in enumerate(products):
        product = product.astype(jnp.bfloat16).astype(jnp.float32)
        for s in range(n_kv):
            for j in range(heads_each):
                proj_send[s, i, j] = product[
                    s * seqs : (s + 1) * seqs, j * size : (j + 1) * size
                ]
    exchange = []
    for r in sorted(range(1, n_kv), key=lambda r: -min(r, n_kv - r)):
        other = lax.rem(kv + r, n_kv)
        exchange.append(
            send(1, r, proj_send.at[other], proj_recv.at[kv], {"kv": other, "tp": tp})
        )
    own = pltpu.make_async_copy(proj_send.at[kv], proj_recv.at[kv], small_sem.at[5])
    own.start()
    floor_load.wait()
    gain_load.wait()
    state_load.wait()
    own.wait()
    for copy in exchange:
        copy.wait_recv()

    for i in range(4):
        for s in range(n_kv):
            for j in range(heads_each):
                piece = proj_recv[s, i, j]
                for b in range(seqs):
                    row = b * heads + s * heads_each + j
                    vectors[i, row : row + 1, :] = piece[b : b + 1, :]

    floor = jnp.concatenate([floor_buf[...]] * seqs, axis=0)
    forget = floor + (1.0 - floor) * jax.nn.sigmoid(vectors[1])
    forget_t = forget.T
    query_t = (vectors[0] * size ** (-0.5)).T
    for b in range(seqs):
        for h in range(heads):
            row = b * heads + h
            f = jnp.broadcast_to(forget_t[:, row : row + 1], (size, size))
            q = jnp.broadcast_to(query_t[:, row : row + 1], (size, size))
            value = vectors[2, row : row + 1, :]
            updated = f * state_buf[b, h] + (1.0 - f) * value
            new_state[b, h] = updated
            head_buf[row : row + 1, :] = jnp.sum(q * updated, axis=0, keepdims=True)
    heads_out = head_buf[...]
    gate = vectors[3]
    branch = (
        heads_out
        * lax.rsqrt(jnp.mean(heads_out * heads_out, axis=-1, keepdims=True) + EPSILON)
        * head_gain_buf[...]
        * (gate * jax.nn.sigmoid(gate))
    )
    branch = branch.astype(jnp.bfloat16).astype(jnp.float32)
    for b in range(seqs):
        for h in range(heads):
            row = b * heads + h
            branch_send[b : b + 1, h * size : (h + 1) * size] = branch[row : row + 1, :]
    branch_copies = [
        send(2, r, branch_send, branch_recv.at[kv, tp], device_of(peer(r)))
        for r in order
    ]
    own_branch = pltpu.make_async_copy(
        branch_send, branch_recv.at[kv, tp], small_sem.at[6]
    )
    own_branch.start()
    out_load.wait()
    own_branch.wait()
    for copy in branch_copies:
        copy.wait_recv()
    for s in range(n_kv):
        for t in range(n_tp):
            branch_all[
                s * seqs : (s + 1) * seqs, t * heads * size : (t + 1) * heads * size
            ] = branch_recv[s, t]
    projected = jnp.dot(
        branch_all[...].astype(jnp.bfloat16),
        out_weight[...],
        preferred_element_type=jnp.float32,
    )
    residual_all[me] = (rows_all[me].astype(jnp.float32) + projected).astype(
        jnp.bfloat16
    )
    residual_copies = [
        send(3, r, residual_all.at[me], residual_all.at[me], device_of(peer(r)))
        for r in order
    ]
    ffn_load.wait()
    for copy in up_loads:
        copy.wait()
    (upward,) = gathered_dot(
        residual_all,
        ffn_gain_buf,
        residual_copies,
        lambda rows_at: [up_weight[rows_at, :]],
    )
    upward = jnp.maximum(upward, 0.0)
    hidden[...] = (upward * upward).astype(jnp.bfloat16)

    for copy in down_loads:
        copy.wait()

    def down(index):
        columns = pl.ds(pl.multiple_of(index * width, width), width)
        return jnp.dot(
            hidden[...], down_weight[:, columns], preferred_element_type=jnp.float32
        )

    sum_copies = []
    for r in order:
        sum_send[r] = down(peer(r)).astype(jnp.bfloat16)
        sum_copies.append(
            send(4, r, sum_send.at[r], sum_recv.at[r], device_of(peer(r)))
        )
    total = down(me)
    for copy in sum_copies:
        copy.wait_recv()
    for r in range(1, group):
        total = total + sum_recv[r].astype(jnp.float32)
    mixed[...] = (residual_all[me].astype(jnp.float32) + total).astype(jnp.bfloat16)
    for copy in sends + exchange + branch_copies + residual_copies + sum_copies:
        copy.wait_send()


def fused_scratch(n_kv, n_tp, tokens, w_query, w_out, w_up, w_down, state):
    group = n_kv * n_tp
    rows, width = tokens.shape
    seqs, heads, size, _ = state.shape
    heads_each = w_query.shape[2] // size
    bf16, f32 = jnp.bfloat16, jnp.float32
    return [
        pltpu.VMEM((group, rows, width), bf16),
        pltpu.VMEM((group, rows, width), bf16),
        pltpu.VMEM((4, w_query.shape[0], w_query.shape[2]), bf16),
        pltpu.VMEM(w_out.shape, bf16),
        pltpu.VMEM(w_up.shape, bf16),
        pltpu.VMEM(w_down.shape, bf16),
        pltpu.VMEM(state.shape, f32),
        pltpu.VMEM((heads, size), f32),
        pltpu.VMEM((1, size), f32),
        pltpu.VMEM((1, group * width), f32),
        pltpu.VMEM((1, group * width), f32),
        pltpu.VMEM((n_kv, 4, heads_each, seqs, size), f32),
        pltpu.VMEM((n_kv, 4, heads_each, seqs, size), f32),
        pltpu.VMEM((4, seqs * heads, size), f32),
        pltpu.VMEM((seqs * heads, size), f32),
        pltpu.VMEM((seqs, heads * size), f32),
        pltpu.VMEM((n_kv, n_tp, seqs, heads * size), f32),
        pltpu.VMEM((rows, n_tp * heads * size), f32),
        pltpu.VMEM((rows, w_up.shape[1]), bf16),
        pltpu.VMEM((group, rows, width), bf16),
        pltpu.VMEM((group, rows, width), bf16),
        pltpu.SemaphoreType.DMA((7,)),
        pltpu.SemaphoreType.DMA((4,)),
        pltpu.SemaphoreType.DMA((1,)),
        pltpu.SemaphoreType.DMA((PIECES,)),
        pltpu.SemaphoreType.DMA((PIECES,)),
        pltpu.SemaphoreType.DMA((1,)),
        pltpu.SemaphoreType.DMA((5, group)),
        pltpu.SemaphoreType.DMA((5, group)),
    ]


def fused(
    tokens,
    w_query,
    w_forget,
    w_input,
    w_output_gate,
    gate_floor,
    head_gain,
    w_out,
    mix_gain,
    ffn_gain,
    w_up,
    w_down,
    state,
):
    n_kv = lax.axis_size("kv")
    n_tp = lax.axis_size("tp")
    anywhere = pl.BlockSpec(memory_space=pl.ANY)
    in_vmem = pl.BlockSpec(memory_space=pltpu.VMEM)
    size = state.shape[2]
    return pl.pallas_call(
        functools.partial(fused_kernel, n_kv, n_tp),
        out_shape=(
            pltpu.VMEM(tokens.shape, jnp.bfloat16),
            pltpu.VMEM(state.shape, jnp.float32),
        ),
        in_specs=[anywhere] * 13,
        out_specs=(in_vmem, in_vmem),
        scratch_shapes=fused_scratch(
            n_kv, n_tp, tokens, w_query, w_out, w_up, w_down, state
        ),
        compiler_params=pltpu.CompilerParams(
            collective_id=0, has_side_effects=True, vmem_limit_bytes=VMEM_BUDGET
        ),
    )(
        tokens,
        w_query[:, 0, :],
        w_forget[:, 0, :],
        w_input[:, 0, :],
        w_output_gate[:, 0, :],
        gate_floor.reshape(state.shape[1], size),
        head_gain.reshape(1, size),
        w_out,
        mix_gain.reshape(1, -1),
        ffn_gain.reshape(1, -1),
        w_up,
        w_down,
        state,
    )


def dispatch(*operands):
    tokens, w_query, w_out, w_up, w_down, state = (
        operands[0],
        operands[1],
        operands[7],
        operands[10],
        operands[11],
        operands[12],
    )
    weights = 2 * (4 * w_query.size + w_out.size + w_up.size + w_down.size)
    held = weights + 4 * state.size + 64 * tokens.size * lax.axis_size("kv")
    size = state.shape[2]
    if (
        held <= VMEM_BUDGET
        and size == LANES
        and w_query.shape[2] % size == 0
        and tokens.shape[0] == lax.axis_size("kv") * state.shape[0]
        and tokens.shape[0] <= 64
    ):
        return fused(*operands)
    return per_device(*operands)


def solution(mesh):
    placed = (
        P("dp", ("kv", "tp")),
        P(None, "tp", "kv"),
        P(None, "tp", "kv"),
        P(None, "tp", "kv"),
        P(None, "tp", "kv"),
        P("tp"),
        P(),
        P(None, ("kv", "tp")),
        P(),
        P(),
        P(None, ("kv", "tp")),
        P(("kv", "tp"), None),
        P(("dp", "kv"), "tp", None, None),
    )
    return jax.shard_map(
        dispatch,
        mesh=mesh,
        in_specs=placed,
        out_specs=(P("dp", ("kv", "tp")), P(("dp", "kv"), "tp", None, None)),
        check_vma=False,
    )
```
